256 devices in a mesh: sp: 64 (over z, y, core), tp: 4 (over x).
Axes of the slice: x: 4, y: 4, z: 8, core: 2. Of those that a mesh axis runs over, the one named last changes fastest.
Arguments:
- tokens: bfloat16 [4, 24576, 2048], P(None, 'sp'), may hold values from -21 to 21
- query_weight: bfloat16 [2048, 1024], P(None, 'tp'), may hold values from -0.125 to 0.125
- key_weight: bfloat16 [2048, 1024], P(None, 'tp'), may hold values from -0.125 to 0.125
- value_weight: bfloat16 [2048, 1024], P(None, 'tp'), may hold values from -0.125 to 0.125
- out_gain: float32 [1024], replicated, may hold values from 0.1 to 1.9
- out_weight: bfloat16 [1024, 2048], P(None, 'tp'), may hold values from -0.1875 to 0.1875
Outputs:
- mixed_out: bfloat16 [4, 24576, 2048], P(None, 'sp', 'tp')
- total_log: float32 [4, 8, 24576], P(None, 'tp', 'sp')
The draws below stay inside these ranges and needn't reach their ends.
All inputs are finite; a program needn't handle non-finite values.
Results may differ from the reference program's by a relative error of at most 0.0098.
Values may be sent and summed in bfloat16 or wider, within the bound.
No kernel may reach another device: no remote copies, remote signals or barrier semaphores. Data moves between devices by JAX's collectives and lax.ppermute only.
A program may use at most 128 MiB of HBM per device.

```python
import jax
import jax.numpy as jnp
from jax import lax

D = 2048
HEADS = 8
HEAD_DIM = 128
REACH = 64
SEQS = 4
TOK_DEV = 384
TOKENS = 24576


def draw_tokens(key, part):
    dims = (SEQS, TOKENS, D)
    return jnp.clip(jax.random.normal(key, dims, jnp.float32), -6.0, 6.0).astype(jnp.bfloat16)


def block_levels(rng, shape, cuts, least, high):
    factor_of, own = 1.0, jax.random.fold_in(rng, 6)
    for axis_at, blocks in cuts:
        heights = jnp.exp(jax.random.uniform(jax.random.fold_in(own, axis_at), (blocks,), jnp.float32, least / len(cuts), high / len(cuts)))
        factor_of = factor_of * jnp.repeat(heights, shape[axis_at] // blocks).reshape([-1 if axis == axis_at else 1 for axis in range(len(shape))])
    return factor_of


def bell_draw(rng, shape, deviation, bound, cuts=(), kind=jnp.bfloat16):
    entries = jax.random.normal(rng, shape, jnp.float32) * deviation
    if len(cuts) > 0:
        entries = block_levels(rng, shape, cuts, -0.22, 0.18) * entries
    return jnp.clip(entries, min=-bound, max=bound).astype(kind)


def setup_inputs(seed: int = 0) -> dict:
    arg_keys = jax.random.split(jax.random.key(seed), 7)
    tokens = draw_tokens(jax.random.fold_in(arg_keys[6], 71), 0)
    query_weight = bell_draw(arg_keys[1], (D, HEADS * HEAD_DIM), D ** -0.5, 0.125, ((1, 4),))
    key_weight = bell_draw(arg_keys[2], (D, HEADS * HEAD_DIM), D ** -0.5, 0.125, ((1, 4),))
    value_weight = bell_draw(arg_keys[3], (D, HEADS * HEAD_DIM), D ** -0.5, 0.125, ((1, 4),))
    out_gain = jnp.clip(1.0 + 0.18 * jax.random.normal(arg_keys[4], (HEADS * HEAD_DIM,), jnp.float32), 0.1, 1.9)
    out_weight = bell_draw(arg_keys[5], (HEADS * HEAD_DIM, D), (HEADS * HEAD_DIM) ** -0.5, 0.1875, ((1, 4),))
    return {"tokens": tokens, "query_weight": query_weight, "key_weight": key_weight, "value_weight": value_weight, "out_gain": out_gain, "out_weight": out_weight}


DILATIONS = (1, 4, 16)
ROPE_BASE = 10000.0
MASK_FILL = -1e+30
NORM_FLOOR = 1e-06

def rotate(projected, positions):
    in_shape = projected.shape
    heads_view = projected.reshape(in_shape[0], in_shape[1], -1, HEAD_DIM)
    half_dim = HEAD_DIM // 2
    frequency = ROPE_BASE ** (-jnp.arange(half_dim, dtype=jnp.float32) / half_dim)
    angles = positions.astype(jnp.float32)[:, None] * frequency[None, :]
    cosine = jnp.cos(angles)[None, :, None, :]
    sine_part = jnp.sin(angles)[None, :, None, :]
    lower_half = heads_view[..., :half_dim]
    upper_half = heads_view[..., half_dim:]
    turned = jnp.concatenate([lower_half * cosine - upper_half * sine_part, upper_half * cosine + lower_half * sine_part], axis=-1)
    return turned.reshape(in_shape)

def band_attend(queries, extended, dilation, offset, total_len):
    seq_count, length, channels = queries.shape
    head_count = channels // HEAD_DIM
    reach_span = REACH * dilation
    query_rows = length // dilation
    key_rows = query_rows + 2 * REACH
    shaped_q = queries.reshape(seq_count, query_rows, dilation, head_count, HEAD_DIM).astype(jnp.float32)
    shaped_k = extended[:, :, :channels].reshape(seq_count, key_rows, dilation, head_count, HEAD_DIM).astype(jnp.float32)
    shaped_v = extended[:, :, channels:].reshape(seq_count, key_rows, dilation, head_count, HEAD_DIM).astype(jnp.float32)
    scores = jnp.einsum('sarhe,sbrhe->srhab', shaped_q, shaped_k)
    query_row = jnp.arange(query_rows, dtype=jnp.int32)[:, None]
    key_row = jnp.arange(key_rows, dtype=jnp.int32)[None, :]
    inband = (key_row >= query_row) & (key_row <= query_row + 2 * REACH)
    residue = jnp.arange(dilation, dtype=jnp.int32)[:, None, None]
    key_pos = offset - reach_span + key_row[None] * dilation + residue
    allowed = inband[None] & (key_pos >= 0) & (key_pos < total_len)
    scores = jnp.where(allowed[None, :, None], scores * HEAD_DIM ** (-0.5), MASK_FILL)
    maximum = lax.optimization_barrier(jnp.max(scores, axis=-1, keepdims=True))
    exp_scores = jnp.exp(scores - maximum)
    weight_sum = lax.optimization_barrier(jnp.sum(exp_scores, axis=-1, keepdims=True))
    probs = lax.optimization_barrier(exp_scores.astype(jnp.bfloat16)).astype(jnp.float32)
    branch = jnp.einsum('srhab,sbrhe->sarhe', probs, shaped_v)
    branch = branch / jnp.transpose(weight_sum, (0, 3, 1, 2, 4))
    branch = branch.reshape(seq_count, length, head_count, HEAD_DIM)
    log_sum = (maximum + jnp.log(weight_sum))[..., 0]
    log_sum = jnp.transpose(log_sum, (0, 2, 3, 1)).reshape(seq_count, head_count, length)
    return (branch, log_sum)

def combine(branch_out, branch_log):
    logs = jnp.stack(branch_log, 0)
    peak = lax.optimization_barrier(jnp.max(logs, axis=0))
    total_log = peak + jnp.log(lax.optimization_barrier(jnp.sum(jnp.exp(logs - peak[None]), axis=0)))
    shares = jnp.exp(logs - total_log[None])
    shares = jnp.transpose(shares, (0, 1, 3, 2))[..., None]
    merged = lax.optimization_barrier(jnp.sum(shares * jnp.stack(branch_out, 0), axis=0))
    seq_count, length, head_count, head_dim = merged.shape
    return (merged.reshape(seq_count, length, head_count * head_dim).astype(jnp.bfloat16), total_log)

def reference(tokens, query_weight, key_weight, value_weight, out_gain, out_weight):
    flat_rows = tokens.reshape(SEQS * TOKENS, D)
    positions = jnp.arange(TOKENS, dtype=jnp.int32)

    def project(weight):
        return jnp.dot(flat_rows, weight, preferred_element_type=jnp.float32).reshape(SEQS, TOKENS, -1)
    queries = rotate(project(query_weight), positions).astype(jnp.bfloat16)
    key_rows = rotate(project(key_weight), positions).astype(jnp.bfloat16)
    values = project(value_weight).astype(jnp.bfloat16)
    wide_span = REACH * DILATIONS[2]
    stacked = jnp.pad(jnp.concatenate([key_rows, values], axis=2), ((0, 0), (wide_span, wide_span), (0, 0)))

    def one_block(block_index):
        row_start = (block_index * TOK_DEV).astype(jnp.int32)
        block_q = lax.dynamic_slice_in_dim(queries, row_start, TOK_DEV, 1)
        branch_out = []
        branch_log = []
        for dilation in DILATIONS:
            reach_span = REACH * dilation
            extended = lax.dynamic_slice_in_dim(stacked, row_start + wide_span - reach_span, TOK_DEV + 2 * reach_span, 1)
            branch, log_sum = band_attend(block_q, extended, dilation, row_start, TOKENS)
            branch_out.append(branch)
            branch_log.append(log_sum)
        return combine(branch_out, branch_log)
    merged, total_log = lax.map(one_block, jnp.arange(TOKENS // TOK_DEV, dtype=jnp.int32))
    merged = jnp.transpose(merged, (1, 0, 2, 3)).reshape(SEQS, TOKENS, HEADS * HEAD_DIM)
    total_log = jnp.transpose(total_log, (1, 2, 0, 3)).reshape(SEQS, HEADS, TOKENS)
    lifted = merged.astype(jnp.float32)
    square = lax.optimization_barrier(jnp.mean(lifted * lifted, axis=-1))
    scaled = (lifted * out_gain.astype(jnp.float32)).astype(jnp.bfloat16)
    projected = jnp.dot(scaled.reshape(SEQS * TOKENS, HEADS * HEAD_DIM), out_weight, preferred_element_type=jnp.float32).reshape(SEQS, TOKENS, D)
    mixed_out = (projected * lax.rsqrt(square + NORM_FLOOR)[..., None]).astype(jnp.bfloat16)
    return (mixed_out, total_log)
```

```python
import math

import jax
import jax.numpy as jnp
from jax import lax
from jax.experimental import pallas as pl
from jax.experimental.pallas import tpu as pltpu
from jax.sharding import PartitionSpec as P

HEAD_DIM = 128
REACH = 64
ROPE_BASE = 10000.0
MASK_FILL = -1e30
NORM_FLOOR = 1e-06

CLASSES = 8
FAR = 16
NEAR = 4
SCALE = HEAD_DIM**-0.5
EXP2_SCALE = SCALE * math.log2(math.e)

CHUNKS = (2, 2)


def shifted(block, axis, distance):
    devices = range(lax.axis_size(axis))
    return lax.ppermute(block, axis, [(i - distance, i) for i in devices if i - distance in devices])


def turned(block, axis, distance):
    size = lax.axis_size(axis)
    return lax.ppermute(block, axis, [(i, (i + distance) % size) for i in range(size)])


def swapped(block, axis):
    return lax.ppermute(block, axis, [(i, i ^ 1) for i in range(lax.axis_size(axis))])


def row_order(length, dtype):
    dims = (CLASSES, length // CLASSES, length)
    wanted = lax.broadcasted_iota(jnp.int32, dims, 1) * CLASSES + lax.broadcasted_iota(jnp.int32, dims, 0)
    hit = lax.broadcasted_iota(jnp.int32, dims, 2) == wanted
    return jnp.where(hit, 1.0, 0.0).reshape(length, length).astype(dtype)


def rotated(projected, cosine, sine):
    heads = []
    for start in range(0, projected.shape[1], HEAD_DIM):
        head = projected[:, start : start + HEAD_DIM]
        heads.append(head * cosine + pltpu.roll(head, HEAD_DIM // 2, 1) * sine)
    return jnp.concatenate(heads, axis=1)


def project_body(turns, tokens_ref, cos_ref, sin_ref, *refs):
    weights, out_ref, order_ref = refs[: len(turns)], refs[-2], refs[-1]
    length = tokens_ref.shape[1]

    @pl.when(pl.program_id(0) == 0)
    def _():
        order_ref[...] = row_order(length, jnp.bfloat16)

    rows = tokens_ref[0]
    at = 0
    for turn, weight in zip(turns, weights):
        made = jnp.dot(rows, weight[...], preferred_element_type=jnp.float32)
        if turn:
            made = rotated(made, cos_ref[...], sin_ref[...])
        width = made.shape[1]
        moved = jnp.dot(order_ref[...], made.astype(jnp.bfloat16), preferred_element_type=jnp.float32)
        moved = moved.astype(jnp.bfloat16).reshape(CLASSES, length // CLASSES, width)
        out_ref[0, :, :, at : at + width] = moved
        at += width


def project(tokens, first, count, cosine, sine, weights, turns):
    _, length, model_dim = tokens.shape
    width = sum(w.shape[1] for w in weights)
    whole = lambda a: pl.BlockSpec(a.shape, lambda s: (0,) * a.ndim)
    return pl.pallas_call(
        lambda *refs: project_body(turns, *refs),
        grid=(count,),
        in_specs=[
            pl.BlockSpec((1, length, model_dim), lambda s: (s + first, 0, 0)),
            whole(cosine),
            whole(sine),
            *[whole(w) for w in weights],
        ],
        out_specs=pl.BlockSpec((1, CLASSES, length // CLASSES, width), lambda s: (s, 0, 0, 0)),
        out_shape=jax.ShapeDtypeStruct((count, CLASSES, length // CLASSES, width), jnp.bfloat16),
        scratch_shapes=[pltpu.VMEM((length, length), jnp.bfloat16)],
        cost_estimate=pl.CostEstimate(
            flops=2 * count * length * model_dim * width,
            transcendentals=0,
            bytes_accessed=2 * (count * length * (model_dim + width) + model_dim * width),
        ),
    )(tokens, cosine, sine, *weights)


def attend_body(
    blocks, place_ref, q_ref, own_ref, first_ref, second_ref, left2_ref, right2_ref, left3_ref, right3_ref,
    out_ref, log_ref, left1, right1, far_bias, near_bias, unit_bias, acc, peak, total, logs, order
):
    per = q_ref.shape[2]
    channels = q_ref.shape[3]
    heads = channels // HEAD_DIM
    reach_far = REACH * FAR // CLASSES
    reach_near = REACH * NEAR // CLASSES
    tile = 16
    start = place_ref[0] * per
    limit = blocks * per
    south = place_ref[1]

    @pl.when(pl.program_id(0) == 0)
    def _():
        order[...] = row_order(CLASSES * per, jnp.bfloat16)

        def filled(ok, row):
            return jnp.where(ok & (row >= 0) & (row < limit), 0.0, MASK_FILL)

        dims = far_bias.shape
        query = lax.broadcasted_iota(jnp.int32, dims, 0)
        key = lax.broadcasted_iota(jnp.int32, dims, 1) - reach_far
        step = key - query
        far_bias[...] = filled((jnp.abs(step) <= reach_far) & ((step & 1) == 0), start + key)
        span = per + 2 * reach_near
        dims = (2, per, 2, span)
        for a in range(2):
            for b in range(2):
                dims = (per, span)
                query = lax.broadcasted_iota(jnp.int32, dims, 0)
                key = lax.broadcasted_iota(jnp.int32, dims, 1) - reach_near
                step = 2 * (key - query) + (b - a)
                near_bias[a * per : (a + 1) * per, b * span : (b + 1) * span] = filled(
                    jnp.abs(step) <= REACH, start + key
                )
        wide = 3 * tile
        dims = (CLASSES, tile, CLASSES * wide)
        query = lax.broadcasted_iota(jnp.int32, dims, 1) * CLASSES + lax.broadcasted_iota(jnp.int32, dims, 0)
        lane = lax.broadcasted_iota(jnp.int32, dims, 2)
        kind = lane // wide
        row = lane - kind * wide - tile
        near = jnp.abs(row * CLASSES + kind - query) <= REACH
        for t in range(per // tile):
            unit_bias[t] = filled(near, start + tile * t + row).reshape(CLASSES * tile, CLASSES * wide)

    left1[...] = jnp.where(south == 1, second_ref[0], first_ref[0])
    right1[...] = jnp.where(south == 1, first_ref[0], second_ref[0])

    def soft(q, k, v, bias):
        scores = lax.dot_general(q, k, (((1,), (1,)), ((), ())), preferred_element_type=jnp.float32) + bias
        top = jnp.max(scores, axis=1, keepdims=True)
        weights = jnp.exp2((scores - top) * EXP2_SCALE)
        weight_sum = jnp.sum(weights, axis=1, keepdims=True)
        summed = jnp.dot(weights.astype(jnp.bfloat16), v, preferred_element_type=jnp.float32)
        return top, weight_sum, summed

    for h in range(heads):
        ql = slice(h * HEAD_DIM, (h + 1) * HEAD_DIM)
        kl = ql
        vl = slice(channels + h * HEAD_DIM, channels + (h + 1) * HEAD_DIM)
        blocks_of = per // tile
        for t in range(blocks_of):
            here = slice(t * tile, (t + 1) * tile)
            lo, hi = tile * (t - 1), tile * (t + 2)

            def around(lanes):
                parts = []
                if lo < 0:
                    parts.append(left1[:, per + lo : per, lanes])
                parts.append(own_ref[0, :, max(lo, 0) : min(hi, per), lanes])
                if hi > per:
                    parts.append(right1[:, 0 : hi - per, lanes])
                joined = jnp.concatenate(parts, axis=1) if len(parts) > 1 else parts[0]
                return joined.reshape(CLASSES * 3 * tile, HEAD_DIM)

            q = q_ref[0, :, here, ql].reshape(CLASSES * tile, HEAD_DIM)
            top, weight_sum, summed = soft(q, around(kl), around(vl), unit_bias[t])
            dims = (CLASSES, tile, HEAD_DIM)
            acc[:, here, :] = summed.reshape(dims)
            peak[:, here, :] = jnp.broadcast_to(top, (CLASSES * tile, HEAD_DIM)).reshape(dims)
            total[:, here, :] = jnp.broadcast_to(weight_sum, (CLASSES * tile, HEAD_DIM)).reshape(dims)
        half = CLASSES // 2
        for c in range(half):

            def around(lanes):
                parts = []
                for r in (c, c + half):
                    parts += [left1[r, per - reach_near : per, lanes], own_ref[0, r, :, lanes], right1[r, 0:reach_near, lanes]]
                return jnp.concatenate(parts, axis=0)

            q = jnp.concatenate([q_ref[0, c, :, ql], q_ref[0, c + half, :, ql]], axis=0)
            top, weight_sum, summed = soft(q, around(kl), around(vl), near_bias[...])
            for n, r in enumerate((c, c + half)):
                rows = slice(n * per, (n + 1) * per)
                old = peak[r]
                new = jnp.maximum(old, top[rows])
                keep = jnp.exp2((old - new) * EXP2_SCALE)
                add = jnp.exp2((top[rows] - new) * EXP2_SCALE)
                acc[r] = acc[r] * keep + summed[rows] * add
                total[r] = total[r] * keep + weight_sum[rows] * add
                peak[r] = new
        for r in range(CLASSES):

            def around(lanes):
                return jnp.concatenate(
                    [
                        left3_ref[0, r, :, lanes],
                        left2_ref[0, r, :, lanes],
                        left1[r, :, lanes],
                        own_ref[0, r, :, lanes],
                        right1[r, :, lanes],
                        right2_ref[0, r, :, lanes],
                        right3_ref[0, r, :, lanes],
                    ],
                    axis=0,
                )

            top, weight_sum, summed = soft(q_ref[0, r, :, ql], around(kl), around(vl), far_bias[...])
            old = peak[r]
            new = jnp.maximum(old, top)
            keep = jnp.exp2((old - new) * EXP2_SCALE)
            add = jnp.exp2((top - new) * EXP2_SCALE)
            whole = total[r] * keep + weight_sum * add
            out_ref[0, r * per : (r + 1) * per, ql] = ((acc[r] * keep + summed * add) / whole).astype(jnp.bfloat16)
            log = new * SCALE + jnp.log(whole)
            rows = slice(r * per, (r + 1) * per)
            if h == 0:
                logs[rows] = log
            else:
                lane = lax.broadcasted_iota(jnp.int32, (per, HEAD_DIM), 1)
                logs[rows] = jnp.where(lane == h, log, logs[rows])
    left = logs[...]
    natural = jnp.zeros((HEAD_DIM, CLASSES * per), jnp.float32)
    for _ in range(3):
        part = left.astype(jnp.bfloat16)
        natural += lax.dot_general(part, order[...], (((0,), (0,)), ((), ())), preferred_element_type=jnp.float32)
        left = left - part.astype(jnp.float32)
    log_ref[0] = natural[0:heads]


def attend(place, blocks, q, first, own, swap_own, swap_far, left2, right2, left3, right3):
    count, classes, per, both = own.shape
    channels = both // 2
    heads = channels // HEAD_DIM
    length = classes * per
    edge = left3.shape[2]
    reach_near = REACH * NEAR // CLASSES
    whole = pl.BlockSpec((1, classes, per, both), lambda s, p: (s, 0, 0, 0))
    part = pl.BlockSpec((1, classes, edge, both), lambda s, p: (s, 0, 0, 0))
    f32 = jnp.float32
    far_keys = per + 2 * REACH * FAR // CLASSES
    near_keys = 2 * (per + 2 * reach_near)
    return pl.pallas_call(
        lambda *refs: attend_body(blocks, *refs),
        grid_spec=pltpu.PrefetchScalarGridSpec(
            num_scalar_prefetch=1,
            grid=(count,),
            in_specs=[
                pl.BlockSpec((1, classes, per, channels), lambda s, p: (s + first, 0, 0, 0)),
                whole, whole, whole, whole, whole, part, part,
            ],
            out_specs=[
                pl.BlockSpec((1, length, channels), lambda s, p: (s, 0, 0)),
                pl.BlockSpec((1, heads, length), lambda s, p: (s, 0, 0)),
            ],
            scratch_shapes=[
                pltpu.VMEM((classes, per, both), jnp.bfloat16),
                pltpu.VMEM((classes, per, both), jnp.bfloat16),
                pltpu.VMEM((per, far_keys), f32),
                pltpu.VMEM((2 * per, near_keys), f32),
                pltpu.VMEM((per // 16, classes * 16, classes * 48), f32),
                pltpu.VMEM((classes, per, HEAD_DIM), f32),
                pltpu.VMEM((classes, per, HEAD_DIM), f32),
                pltpu.VMEM((classes, per, HEAD_DIM), f32),
                pltpu.VMEM((length, HEAD_DIM), f32),
                pltpu.VMEM((length, length), jnp.bfloat16),
            ],
        ),
        out_shape=[
            jax.ShapeDtypeStruct((count, length, channels), jnp.bfloat16),
            jax.ShapeDtypeStruct((count, heads, length), f32),
        ],
        cost_estimate=pl.CostEstimate(
            flops=4 * count * length * channels * (far_keys + near_keys + 3 * classes * 48) * 4,
            transcendentals=count * heads * length * 800,
            bytes_accessed=2 * count * length * both * 6,
        ),
    )(place, q, own, swap_own, swap_far, left2, right2, left3, right3)


def finish_body(channels_all, place_ref, *refs):
    parts, gains, weights = refs[0:5], refs[5:9], refs[9:13]
    out_ref, order = refs[13], refs[14]
    own, before, after, low, high = parts
    length = own.shape[1]

    @pl.when(pl.program_id(0) == 0)
    def _():
        order[...] = row_order(length, jnp.bfloat16)

    opposite = jnp.concatenate([low[0], high[0]], axis=0)
    projected = None
    square = None
    for value, gain, weight in zip((own[0], before[0], after[0], opposite), gains, weights):
        lifted = value.astype(jnp.float32)
        scaled = (lifted * gain[...]).astype(jnp.bfloat16)
        term = jnp.dot(scaled, weight[...], preferred_element_type=jnp.float32)
        squares = jnp.sum(lifted * lifted, axis=1, keepdims=True)
        projected = term if projected is None else projected + term
        square = squares if square is None else square + squares
    mixed = (projected * lax.rsqrt(square / channels_all + NORM_FLOOR)).astype(jnp.bfloat16)
    natural = lax.dot_general(order[...], mixed, (((0,), (0,)), ((), ())), preferred_element_type=jnp.float32)
    out_ref[0] = natural.astype(jnp.bfloat16)


def finish(place, merged, before, after, low, high, gain, weight, ranks):
    count, length, channels = merged.shape
    half = length // 2
    channels_all, width = weight.shape
    block = pl.BlockSpec((1, length, channels), lambda s, p: (s, 0, 0))
    part = pl.BlockSpec((1, half, channels), lambda s, p: (s, 0, 0))
    turns = (0, ranks - 1, 1, 2)

    def gain_at(turn):
        return pl.BlockSpec((1, channels), lambda s, p: (0, lax.rem(p[2] + turn, ranks)))

    def weight_at(turn):
        return pl.BlockSpec((channels, width), lambda s, p: (lax.rem(p[2] + turn, ranks), 0))

    return pl.pallas_call(
        lambda *refs: finish_body(channels_all, *refs),
        grid_spec=pltpu.PrefetchScalarGridSpec(
            num_scalar_prefetch=1,
            grid=(count,),
            in_specs=[block, block, block, part, part, *map(gain_at, turns), *map(weight_at, turns)],
            out_specs=pl.BlockSpec((1, length, width), lambda s, p: (s, 0, 0)),
            scratch_shapes=[pltpu.VMEM((length, length), jnp.bfloat16)],
        ),
        out_shape=jax.ShapeDtypeStruct((count, length, width), jnp.bfloat16),
        cost_estimate=pl.CostEstimate(
            flops=2 * count * length * channels_all * width,
            transcendentals=0,
            bytes_accessed=2 * (count * length * (channels_all + width) + channels_all * width),
        ),
    )(place, merged, before, after, low, high, *[gain] * 4, *[weight] * 4)


def shards(tokens, query_weight, key_weight, value_weight, out_gain, out_weight):
    seq_count, length, model_dim = tokens.shape
    at = lax.axis_index("sp")
    core = at % 2
    rank = lax.axis_index("tp")
    ranks = lax.axis_size("tp")
    blocks = lax.axis_size("sp")
    place = jnp.stack([at, 1 - core, rank]).astype(jnp.int32)
    positions = at * length + jnp.arange(length, dtype=jnp.int32)
    half_dim = HEAD_DIM // 2
    frequency = ROPE_BASE ** (-jnp.arange(half_dim, dtype=jnp.float32) / half_dim)
    angles = positions.astype(jnp.float32)[:, None] * frequency[None, :]
    cosine = jnp.cos(angles)
    sine = jnp.sin(angles)
    cosine = jnp.concatenate([cosine, cosine], axis=1)
    sine = jnp.concatenate([-sine, sine], axis=1)
    per = length // CLASSES
    edge = REACH * FAR // CLASSES - 2 * per

    gain = out_gain.reshape(1, -1)
    mixed_all, logs_all = [], []
    first = 0
    stage = []
    for count in CHUNKS:
        own = project(tokens, first, count, cosine, sine, (key_weight, value_weight), (True, False))
        left2 = shifted(own, "sp", 2)
        right2 = shifted(own, "sp", -2)
        swap_own = swapped(own, "sp")
        stage.append((first, count, own, left2, right2, swap_own))
        first += count
    queries = project(tokens, 0, seq_count, cosine, sine, (query_weight,), (True,))
    for first, count, own, left2, right2, swap_own in stage:
        swap_far = swapped(jnp.where(core == 1, left2, right2), "sp")
        left3 = shifted(left2[:, :, per - edge :], "sp", 1)
        right3 = shifted(right2[:, :, :edge], "sp", -1)
        merged, logs = attend(
            place, blocks, queries, first, own, swap_own, swap_far, left2, right2, left3, right3
        )
        before = turned(merged, "tp", 1)
        after = turned(merged, "tp", -1)
        low = turned(before[:, : length // 2], "tp", 1)
        high = turned(after[:, length // 2 :], "tp", -1)
        mixed_all.append(finish(place, merged, before, after, low, high, gain, out_weight, ranks))
        logs_all.append(logs)
    return (jnp.concatenate(mixed_all, axis=0), jnp.concatenate(logs_all, axis=0))


def solution(mesh):
    return jax.shard_map(
        shards,
        mesh=mesh,
        in_specs=(
            P(None, "sp", None),
            P(None, "tp"),
            P(None, "tp"),
            P(None, "tp"),
            P(),
            P(None, "tp"),
        ),
        out_specs=(P(None, "sp", "tp"), P(None, "tp", "sp")),
        check_vma=False,
    )
```

```python
import math

import jax
import jax.numpy as jnp
from jax import lax
from jax.experimental import pallas as pl
from jax.experimental.pallas import tpu as pltpu
from jax.sharding import PartitionSpec as P

HEAD_DIM = 128
REACH = 64
ROPE_BASE = 10000.0
MASK_FILL = -1e30
NORM_FLOOR = 1e-06

CLASSES = 8
FAR = 16
NEAR = 4
SCALE = HEAD_DIM**-0.5
EXP2_SCALE = SCALE * math.log2(math.e)

CHUNKS = (2, 2)


def shifted(block, axis, distance):
    devices = range(lax.axis_size(axis))
    return lax.ppermute(block, axis, [(i - distance, i) for i in devices if i - distance in devices])


def turned(block, axis, distance):
    size = lax.axis_size(axis)
    return lax.ppermute(block, axis, [(i, (i + distance) % size) for i in range(size)])


def swapped(block, axis):
    return lax.ppermute(block, axis, [(i, i ^ 1) for i in range(lax.axis_size(axis))])


def row_order(length, dtype):
    dims = (CLASSES, length // CLASSES, length)
    wanted = lax.broadcasted_iota(jnp.int32, dims, 1) * CLASSES + lax.broadcasted_iota(jnp.int32, dims, 0)
    hit = lax.broadcasted_iota(jnp.int32, dims, 2) == wanted
    return jnp.where(hit, 1.0, 0.0).reshape(length, length).astype(dtype)


def rotated(projected, cosine, sine):
    heads = []
    for start in range(0, projected.shape[1], HEAD_DIM):
        head = projected[:, start : start + HEAD_DIM]
        heads.append(head * cosine + pltpu.roll(head, HEAD_DIM // 2, 1) * sine)
    return jnp.concatenate(heads, axis=1)


PIECES = 2


def project_body(*refs):
    pieces, refs = refs[:PIECES], refs[PIECES:]
    cos_ref, sin_ref, query_ref, key_ref, value_ref, q_ref, kv_ref, order_ref = refs
    length = cos_ref.shape[0]
    width = query_ref.shape[1]

    @pl.when(pl.program_id(0) == 0)
    def _():
        order_ref[...] = row_order(length, jnp.bfloat16)

    def made(weight):
        return jnp.concatenate(
            [jnp.dot(p[0], weight[...], preferred_element_type=jnp.float32) for p in pieces], axis=0
        )

    def moved(value):
        value = jnp.dot(order_ref[...], value.astype(jnp.bfloat16), preferred_element_type=jnp.float32)
        return value.astype(jnp.bfloat16).reshape(CLASSES, length // CLASSES, width)

    keys = made(key_ref)
    values = made(value_ref)
    queries = made(query_ref)
    kv_ref[0, :, :, :width] = moved(rotated(keys, cos_ref[...], sin_ref[...]))
    kv_ref[0, :, :, width:] = moved(values)
    q_ref[0] = moved(rotated(queries, cos_ref[...], sin_ref[...]))


def project(tokens, first, count, cosine, sine, query_weight, key_weight, value_weight):
    _, length, model_dim = tokens.shape
    width = query_weight.shape[1]
    weights = (query_weight, key_weight, value_weight)
    rows = length // PIECES
    whole = lambda a: pl.BlockSpec(a.shape, lambda s: (0,) * a.ndim)
    made = lambda wide: pl.BlockSpec((1, CLASSES, length // CLASSES, wide), lambda s: (s, 0, 0, 0))
    piece = lambda n: pl.BlockSpec((1, rows, model_dim), lambda s: (s + first, n, 0))
    return pl.pallas_call(
        project_body,
        grid=(count,),
        in_specs=[*map(piece, range(PIECES)), whole(cosine), whole(sine), *[whole(w) for w in weights]],
        out_specs=[made(width), made(2 * width)],
        out_shape=[
            jax.ShapeDtypeStruct((count, CLASSES, length // CLASSES, wide), jnp.bfloat16)
            for wide in (width, 2 * width)
        ],
        scratch_shapes=[pltpu.VMEM((length, length), jnp.bfloat16)],
        cost_estimate=pl.CostEstimate(
            flops=6 * count * length * model_dim * width,
            transcendentals=0,
            bytes_accessed=2 * (count * length * (model_dim + 3 * width) + 3 * model_dim * width),
        ),
    )(*[tokens] * PIECES, cosine, sine, *weights)


def attend_body(
    blocks, place_ref, q_ref, own_ref, first_ref, second_ref, left2_ref, right2_ref, left3_ref, right3_ref,
    out_ref, log_ref, left1, right1, far_bias, near_bias, unit_bias,
    raw_unit, raw_near, raw_far, probs_unit, probs_near, probs_far, acc, peak, total, logs, order
):
    per = q_ref.shape[2]
    channels = q_ref.shape[3]
    heads = channels // HEAD_DIM
    reach_far = REACH * FAR // CLASSES
    reach_near = REACH * NEAR // CLASSES
    tile = 16
    start = place_ref[0] * per
    limit = blocks * per
    south = place_ref[1]
    raw = (raw_unit, raw_near, raw_far)
    probs = (probs_unit, probs_near, probs_far)

    @pl.when(pl.program_id(0) == 0)
    def _():
        order[...] = row_order(CLASSES * per, jnp.bfloat16)

        def filled(ok, row):
            return jnp.where(ok & (row >= 0) & (row < limit), 0.0, MASK_FILL)

        dims = far_bias.shape
        query = lax.broadcasted_iota(jnp.int32, dims, 0)
        key = lax.broadcasted_iota(jnp.int32, dims, 1) - reach_far
        step = key - query
        far_bias[...] = filled((jnp.abs(step) <= reach_far) & ((step & 1) == 0), start + key)
        span = per + 2 * reach_near
        dims = (2, per, 2, span)
        for a in range(2):
            for b in range(2):
                dims = (per, span)
                query = lax.broadcasted_iota(jnp.int32, dims, 0)
                key = lax.broadcasted_iota(jnp.int32, dims, 1) - reach_near
                step = 2 * (key - query) + (b - a)
                near_bias[a * per : (a + 1) * per, b * span : (b + 1) * span] = filled(
                    jnp.abs(step) <= REACH, start + key
                )
        wide = 3 * tile
        dims = (CLASSES, tile, CLASSES * wide)
        query = lax.broadcasted_iota(jnp.int32, dims, 1) * CLASSES + lax.broadcasted_iota(jnp.int32, dims, 0)
        lane = lax.broadcasted_iota(jnp.int32, dims, 2)
        kind = lane // wide
        row = lane - kind * wide - tile
        near = jnp.abs(row * CLASSES + kind - query) <= REACH
        for t in range(per // tile):
            unit_bias[t] = filled(near, start + tile * t + row).reshape(CLASSES * tile, CLASSES * wide)

    left1[...] = jnp.where(south == 1, second_ref[0], first_ref[0])
    right1[...] = jnp.where(south == 1, first_ref[0], second_ref[0])

    half = CLASSES // 2
    slabs = per // tile

    def near_unit(lanes, t):
        lo, hi = tile * (t - 1), tile * (t + 2)
        parts = []
        if lo < 0:
            parts.append(left1[:, per + lo : per, lanes])
        parts.append(own_ref[0, :, max(lo, 0) : min(hi, per), lanes])
        if hi > per:
            parts.append(right1[:, 0 : hi - per, lanes])
        joined = jnp.concatenate(parts, axis=1) if len(parts) > 1 else parts[0]
        return joined.reshape(CLASSES * 3 * tile, HEAD_DIM)

    def near_pair(lanes, c):
        parts = []
        for r in (c, c + half):
            parts += [left1[r, per - reach_near : per, lanes], own_ref[0, r, :, lanes], right1[r, 0:reach_near, lanes]]
        return jnp.concatenate(parts, axis=0)

    def near_far(lanes, r):
        parts = [left3_ref[0, r, :, lanes], left2_ref[0, r, :, lanes], left1[r, :, lanes], own_ref[0, r, :, lanes]]
        parts += [right1[r, :, lanes], right2_ref[0, r, :, lanes], right3_ref[0, r, :, lanes]]
        return jnp.concatenate(parts, axis=0)

    keys_of = (near_unit, near_pair, near_far)

    def queries_of(kind, lanes, b):
        if kind == 0:
            return q_ref[0, :, b * tile : (b + 1) * tile, lanes].reshape(CLASSES * tile, HEAD_DIM)
        if kind == 1:
            return jnp.concatenate([q_ref[0, b, :, lanes], q_ref[0, b + half, :, lanes]], axis=0)
        return q_ref[0, b, :, lanes]

    def bias_of(kind, b):
        return (unit_bias, near_bias, far_bias)[kind][b] if kind == 0 else (near_bias, far_bias)[kind - 1][...]

    def score(h, kind, b):
        lanes = slice(h * HEAD_DIM, (h + 1) * HEAD_DIM)
        made = lax.dot_general(
            queries_of(kind, lanes, b), keys_of[kind](lanes, b), (((1,), (1,)), ((), ())),
            preferred_element_type=jnp.float32,
        )
        raw[kind][h, b] = made + bias_of(kind, b)

    def weigh(h, kind, b):
        scores = raw[kind][h, b]
        top = jnp.max(scores, axis=1, keepdims=True)
        weights = jnp.exp2((scores - top) * EXP2_SCALE)
        weight_sum = jnp.sum(weights, axis=1, keepdims=True)
        probs[kind][h, b] = weights.astype(jnp.bfloat16)
        rows = scores.shape[0]
        put(peak, h, kind, b, jnp.broadcast_to(top, (rows, HEAD_DIM)))
        put(total, h, kind, b, jnp.broadcast_to(weight_sum, (rows, HEAD_DIM)))

    def put(ref, h, kind, b, value):
        if kind == 0:
            ref[h, 0, :, b * tile : (b + 1) * tile, :] = value.reshape(CLASSES, tile, HEAD_DIM)
        elif kind == 1:
            ref[h, 1, b] = value[:per]
            ref[h, 1, b + half] = value[per:]
        else:
            ref[h, 2, b] = value

    def blend(h, kind, b):
        lanes = slice(channels + h * HEAD_DIM, channels + (h + 1) * HEAD_DIM)
        summed = jnp.dot(probs[kind][h, b], keys_of[kind](lanes, b), preferred_element_type=jnp.float32)
        if kind < 2:
            put(acc, h, kind, b, summed)
            return
        tops = [peak[h, k, b] for k in range(3)]
        new = jnp.maximum(jnp.maximum(tops[0], tops[1]), tops[2])
        shares = [jnp.exp2((top - new) * EXP2_SCALE) for top in tops]
        whole = total[h, 0, b] * shares[0] + total[h, 1, b] * shares[1] + total[h, 2, b] * shares[2]
        value = acc[h, 0, b] * shares[0] + acc[h, 1, b] * shares[1] + summed * shares[2]
        rows = slice(b * per, (b + 1) * per)
        out_ref[0, rows, h * HEAD_DIM : (h + 1) * HEAD_DIM] = (value / whole).astype(jnp.bfloat16)
        log = new * SCALE + jnp.log(whole)
        if h == 0:
            logs[rows] = log
        else:
            lane = lax.broadcasted_iota(jnp.int32, (per, HEAD_DIM), 1)
            logs[rows] = jnp.where(lane == h, log, logs[rows])

    units = []
    for h in range(heads):
        units.append([(h, 0, t) for t in range(slabs)])
        units.append([(h, 1, c) for c in range(half)])
        units.append([(h, 2, r) for r in range(half)])
        units.append([(h, 2, r) for r in range(half, CLASSES)])
    for step in range(len(units) + 2):
        for stage, lag in ((score, 0), (blend, 2), (weigh, 1)):
            if 0 <= step - lag < len(units):
                for item in units[step - lag]:
                    stage(*item)
    left = logs[...]
    natural = jnp.zeros((HEAD_DIM, CLASSES * per), jnp.float32)
    for _ in range(3):
        part = left.astype(jnp.bfloat16)
        natural += lax.dot_general(part, order[...], (((0,), (0,)), ((), ())), preferred_element_type=jnp.float32)
        left = left - part.astype(jnp.float32)
    log_ref[0] = natural[0:heads]


def attend(place, blocks, q, own, swap_own, swap_far, left2, right2, left3, right3):
    count, classes, per, both = own.shape
    channels = both // 2
    heads = channels // HEAD_DIM
    length = classes * per
    edge = left3.shape[2]
    reach_near = REACH * NEAR // CLASSES
    whole = pl.BlockSpec((1, classes, per, both), lambda s, p: (s, 0, 0, 0))
    part = pl.BlockSpec((1, classes, edge, both), lambda s, p: (s, 0, 0, 0))
    f32 = jnp.float32
    far_keys = per + 2 * REACH * FAR // CLASSES
    near_keys = 2 * (per + 2 * reach_near)
    blocks_of = (
        (heads, per // 16, classes * 16, classes * 48),
        (heads, classes // 2, 2 * per, near_keys),
        (heads, classes, per, far_keys),
    )
    return pl.pallas_call(
        lambda *refs: attend_body(blocks, *refs),
        grid_spec=pltpu.PrefetchScalarGridSpec(
            num_scalar_prefetch=1,
            grid=(count,),
            in_specs=[
                pl.BlockSpec((1, classes, per, channels), lambda s, p: (s, 0, 0, 0)),
                whole, whole, whole, whole, whole, part, part,
            ],
            out_specs=[
                pl.BlockSpec((1, length, channels), lambda s, p: (s, 0, 0)),
                pl.BlockSpec((1, heads, length), lambda s, p: (s, 0, 0)),
            ],
            scratch_shapes=[
                pltpu.VMEM((classes, per, both), jnp.bfloat16),
                pltpu.VMEM((classes, per, both), jnp.bfloat16),
                pltpu.VMEM((per, far_keys), f32),
                pltpu.VMEM((2 * per, near_keys), f32),
                pltpu.VMEM((per // 16, classes * 16, classes * 48), f32),
                *[pltpu.VMEM(dims, dtype) for dtype in (f32, jnp.bfloat16) for dims in blocks_of],
                pltpu.VMEM((heads, 2, classes, per, HEAD_DIM), f32),
                pltpu.VMEM((heads, 3, classes, per, HEAD_DIM), f32),
                pltpu.VMEM((heads, 3, classes, per, HEAD_DIM), f32),
                pltpu.VMEM((length, HEAD_DIM), f32),
                pltpu.VMEM((length, length), jnp.bfloat16),
            ],
        ),
        out_shape=[
            jax.ShapeDtypeStruct((count, length, channels), jnp.bfloat16),
            jax.ShapeDtypeStruct((count, heads, length), f32),
        ],
        cost_estimate=pl.CostEstimate(
            flops=4 * count * length * channels * (far_keys + near_keys + 3 * classes * 48) * 4,
            transcendentals=count * heads * length * 800,
            bytes_accessed=2 * count * length * both * 6,
        ),
    )(place, q, own, swap_own, swap_far, left2, right2, left3, right3)


def finish_body(channels_all, place_ref, *refs):
    parts, gains, weights = refs[0:5], refs[5:9], refs[9:13]
    out_ref, order = refs[13], refs[14]
    own, before, after, low, high = parts
    length = own.shape[1]

    @pl.when(pl.program_id(0) == 0)
    def _():
        order[...] = row_order(length, jnp.bfloat16)

    opposite = jnp.concatenate([low[0], high[0]], axis=0)
    projected = None
    square = None
    for value, gain, weight in zip((own[0], before[0], after[0], opposite), gains, weights):
        lifted = value.astype(jnp.float32)
        scaled = (lifted * gain[...]).astype(jnp.bfloat16)
        term = jnp.dot(scaled, weight[...], preferred_element_type=jnp.float32)
        squares = jnp.sum(lifted * lifted, axis=1, keepdims=True)
        projected = term if projected is None else projected + term
        square = squares if square is None else square + squares
    mixed = (projected * lax.rsqrt(square / channels_all + NORM_FLOOR)).astype(jnp.bfloat16)
    natural = lax.dot_general(order[...], mixed, (((0,), (0,)), ((), ())), preferred_element_type=jnp.float32)
    out_ref[0] = natural.astype(jnp.bfloat16)


def finish(place, merged, before, after, low, high, gain, weight, ranks):
    count, length, channels = merged.shape
    half = length // 2
    channels_all, width = weight.shape
    block = pl.BlockSpec((1, length, channels), lambda s, p: (s, 0, 0))
    part = pl.BlockSpec((1, half, channels), lambda s, p: (s, 0, 0))
    turns = (0, ranks - 1, 1, 2)

    def gain_at(turn):
        return pl.BlockSpec((1, channels), lambda s, p: (0, lax.rem(p[2] + turn, ranks)))

    def weight_at(turn):
        return pl.BlockSpec((channels, width), lambda s, p: (lax.rem(p[2] + turn, ranks), 0))

    return pl.pallas_call(
        lambda *refs: finish_body(channels_all, *refs),
        grid_spec=pltpu.PrefetchScalarGridSpec(
            num_scalar_prefetch=1,
            grid=(count,),
            in_specs=[block, block, block, part, part, *map(gain_at, turns), *map(weight_at, turns)],
            out_specs=pl.BlockSpec((1, length, width), lambda s, p: (s, 0, 0)),
            scratch_shapes=[pltpu.VMEM((length, length), jnp.bfloat16)],
        ),
        out_shape=jax.ShapeDtypeStruct((count, length, width), jnp.bfloat16),
        cost_estimate=pl.CostEstimate(
            flops=2 * count * length * channels_all * width,
            transcendentals=0,
            bytes_accessed=2 * (count * length * (channels_all + width) + channels_all * width),
        ),
    )(place, merged, before, after, low, high, *[gain] * 4, *[weight] * 4)


def shards(tokens, query_weight, key_weight, value_weight, out_gain, out_weight):
    seq_count, length, model_dim = tokens.shape
    at = lax.axis_index("sp")
    core = at % 2
    rank = lax.axis_index("tp")
    ranks = lax.axis_size("tp")
    blocks = lax.axis_size("sp")
    place = jnp.stack([at, 1 - core, rank]).astype(jnp.int32)
    positions = at * length + jnp.arange(length, dtype=jnp.int32)
    half_dim = HEAD_DIM // 2
    frequency = ROPE_BASE ** (-jnp.arange(half_dim, dtype=jnp.float32) / half_dim)
    angles = positions.astype(jnp.float32)[:, None] * frequency[None, :]
    cosine = jnp.cos(angles)
    sine = jnp.sin(angles)
    cosine = jnp.concatenate([cosine, cosine], axis=1)
    sine = jnp.concatenate([-sine, sine], axis=1)
    per = length // CLASSES
    edge = REACH * FAR // CLASSES - 2 * per

    gain = out_gain.reshape(1, -1)
    mixed_all, logs_all = [], []
    first = 0
    stage = []
    for count in CHUNKS:
        queries, own = project(tokens, first, count, cosine, sine, query_weight, key_weight, value_weight)
        left2 = shifted(own, "sp", 2)
        right2 = shifted(own, "sp", -2)
        swap_own = swapped(own, "sp")
        stage.append((queries, own, left2, right2, swap_own))
        first += count
    for queries, own, left2, right2, swap_own in stage:
        swap_far = swapped(jnp.where(core == 1, left2, right2), "sp")
        left3 = shifted(left2[:, :, per - edge :], "sp", 1)
        right3 = shifted(right2[:, :, :edge], "sp", -1)
        merged, logs = attend(
            place, blocks, queries, own, swap_own, swap_far, left2, right2, left3, right3
        )
        before = turned(merged, "tp", 1)
        after = turned(merged, "tp", -1)
        low = turned(before[:, : length // 2], "tp", 1)
        high = turned(after[:, length // 2 :], "tp", -1)
        mixed_all.append(finish(place, merged, before, after, low, high, gain, out_weight, ranks))
        logs_all.append(logs)
    return (jnp.concatenate(mixed_all, axis=0), jnp.concatenate(logs_all, axis=0))


def solution(mesh):
    return jax.shard_map(
        shards,
        mesh=mesh,
        in_specs=(
            P(None, "sp", None),
            P(None, "tp"),
            P(None, "tp"),
            P(None, "tp"),
            P(),
            P(None, "tp"),
        ),
        out_specs=(P(None, "sp", "tp"), P(None, "tp", "sp")),
        check_vma=False,
    )
```
